32 devices in a mesh: kv: 8 (over z, x), tp: 4 (over y, core).
Axes of the slice: x: 2, y: 2, z: 4, core: 2. Of those that a mesh axis runs over, the one named last changes fastest.
Arguments:
- hidden_in: bfloat16 [16, 4096], P(None, ('kv', 'tp')), may hold values from -5 to 5
- pre_gain: float32 [4096], P('kv'), may hold values from 0.1 to 1.9
- w_query: bfloat16 [4096, 3072], P('kv', 'tp'), may hold values from -0.09375 to 0.09375
- w_key: bfloat16 [4096, 1024], P('kv', 'tp'), may hold values from -0.09375 to 0.09375
- w_value: bfloat16 [4096, 1024], P('kv', 'tp'), may hold values from -0.09375 to 0.09375
- w_forget: bfloat16 [4096, 16], P('kv'), may hold values from -0.09375 to 0.09375
- forget_bias: float32 [16], P('tp'), may hold values from -2 to 1.5
- key_cache: bfloat16 [16, 8192, 1024], P(None, 'kv', 'tp'), may hold values from -1300 to 1300
- value_cache: bfloat16 [16, 8192, 1024], P(None, 'kv', 'tp'), may hold values from -6 to 6
- decay_to_end: float32 [16, 16, 8192], P(None, 'tp', 'kv'), may hold values from -8194 to 0, as said below
- w_output: bfloat16 [3072, 4096], P('tp', 'kv'), may hold values from -0.109375 to 0.109375
- mid_gain: float32 [4096], P('kv'), may hold values from 0.1 to 1.9
- w_gate: bfloat16 [4096, 11264], P('kv', 'tp'), may hold values from -0.09375 to 0.09375
- w_up: bfloat16 [4096, 11264], P('kv', 'tp'), may hold values from -0.09375 to 0.09375
- w_down: bfloat16 [11264, 4096], P('tp', 'kv'), may hold values from -0.0546875 to 0.0546875
Outputs:
- updated: float32 [16, 4096], P(None, ('kv', 'tp'))
The draws below stay inside these ranges and needn't reach their ends.
Inputs may be any that keep to these rules, and one draw needn't show every extreme that they name: `decay_to_end`: never falls toward later positions and is 0 at the last cached position.
All inputs are finite; a program needn't handle non-finite values.
Results may differ from the reference program's by a relative error of at most 0.028.
Values may be sent and summed in bfloat16 or wider, within the bound.
No kernel may reach another device: no remote copies, remote signals or barrier semaphores. Data moves between devices by JAX's collectives and lax.ppermute only.
A program may use at most 128 MiB of HBM per device.

```python
import jax
import jax.numpy as jnp
from jax import lax

D = 4096
QH = 48
KEY_VALUE_HEADS = 16
HD = 64
FF = 11264
BATCH_SEQUENCES = 16
POS_DEV = 1024
CACHE_LENGTH = 8192
N_KV = 8
N_TP = 4


def draw_hidden_in(key, part):
    key_base, key_rough = jax.random.split(key, 2)
    column = jnp.arange(D).astype(jnp.float32)
    span = D // N_KV
    rise = column / D + column % span / span
    rough = jnp.exp(jax.random.uniform(key_rough, (D,), minval=-0.7, maxval=0.7))
    scale = jnp.exp(jnp.log(3.0) * rise) * rough
    base = jnp.clip(jax.random.normal(key_base, (BATCH_SEQUENCES, D)), -5.0, 5.0)
    return (0.05 * base * scale[None, :]).astype(jnp.bfloat16)


def draw_key_cache(key, part):
    key_base = jax.random.fold_in(key, 0)
    result = jnp.clip(jax.random.normal(key_base, (BATCH_SEQUENCES, CACHE_LENGTH, KEY_VALUE_HEADS, HD)), -6.0, 6.0)
    return result.reshape(BATCH_SEQUENCES, CACHE_LENGTH, KEY_VALUE_HEADS * HD).astype(jnp.bfloat16)


def draw_decay_to_end(key, part):
    key_entries = jax.random.split(key, 7)
    slow_share = 0.5
    sluggish_flag = jax.random.uniform(key_entries[0], (KEY_VALUE_HEADS,)) < slow_share
    total = jnp.exp(jax.random.uniform(key_entries[1], (KEY_VALUE_HEADS,), minval=jnp.log(0.2), maxval=jnp.log(0.8)))
    fast_len = jnp.exp(jax.random.uniform(key_entries[2], (KEY_VALUE_HEADS,), minval=jnp.log(30.0), maxval=jnp.log(100.0)))
    mean_rate = jnp.where(sluggish_flag, total / CACHE_LENGTH, 1.0 / fast_len)
    shard_factor = jnp.exp(jax.random.uniform(key_entries[3], (BATCH_SEQUENCES, KEY_VALUE_HEADS, N_KV), minval=-0.7, maxval=0.7))
    block_of = jnp.arange(CACHE_LENGTH) // POS_DEV
    shard_pos = jnp.take(shard_factor, block_of, axis=2)
    rough = jnp.exp(jax.random.uniform(key_entries[4], (BATCH_SEQUENCES, KEY_VALUE_HEADS, CACHE_LENGTH), minval=jnp.log(0.3), maxval=jnp.log(3.0)))
    decode_steps = -mean_rate[None, :, None] * shard_pos * rough
    spike_offset = jax.random.randint(key_entries[5], (BATCH_SEQUENCES, KEY_VALUE_HEADS, 2), 0, CACHE_LENGTH)
    spike_length = jnp.log(jax.random.uniform(key_entries[6], (BATCH_SEQUENCES, KEY_VALUE_HEADS, 2), minval=0.55, maxval=0.8))
    decode_position = jnp.arange(CACHE_LENGTH)
    spike_count = jnp.where(decode_position[None, None, :] == spike_offset[:, :, 0:1], spike_length[:, :, 0:1], 0.0)
    spike_count = spike_count + jnp.where(decode_position[None, None, :] == spike_offset[:, :, 1:2], spike_length[:, :, 1:2], 0.0)
    decode_steps = decode_steps + jnp.where(sluggish_flag[None, :, None], spike_count, 0.0)
    later = jnp.cumsum(decode_steps[:, :, ::-1], axis=2)[:, :, ::-1] - decode_steps
    return later.astype(jnp.float32)


def steps_of(own_key, dims, shards, low, top_value):
    gain, own = 1.0, jax.random.fold_in(own_key, 6)
    for position, blocks in shards:
        heights = jnp.exp(jax.random.uniform(jax.random.fold_in(own, position), (blocks,), jnp.float32, low / len(shards), top_value / len(shards)))
        gain = gain * jnp.repeat(heights, dims[position] // blocks).reshape([-1 if axis == position else 1 for axis in range(len(dims))])
    return gain


def centred(key, dims, width, reach, cuts=(), kind=jnp.bfloat16):
    values = jax.random.normal(key, dims, jnp.float32) * width
    if len(cuts) > 0:
        values = steps_of(key, dims, cuts, -0.22, 0.18) * values
    return jnp.clip(values, min=-reach, max=reach).astype(kind)


def setup_inputs(seed: int = 0) -> dict:
    key_of = jax.random.split(jax.random.key(seed), 16)
    hidden_in = draw_hidden_in(jax.random.fold_in(key_of[15], 71), 0)
    pre_gain = jnp.clip(1.0 + 0.18 * jax.random.normal(key_of[1], (D,), jnp.float32), 0.1, 1.9)
    w_query = centred(key_of[2], (D, QH * HD), D ** -0.5, 0.09375, ((0, 8), (1, 4)))
    w_key = centred(key_of[3], (D, KEY_VALUE_HEADS * HD), D ** -0.5, 0.09375, ((0, 8), (1, 4)))
    w_value = centred(key_of[4], (D, KEY_VALUE_HEADS * HD), D ** -0.5, 0.09375, ((0, 8), (1, 4)))
    w_forget = centred(key_of[5], (D, KEY_VALUE_HEADS), D ** -0.5, 0.09375, ((0, 8),))
    forget_bias = jnp.clip(-2.0 + 3.5 * jax.random.uniform(key_of[6], (KEY_VALUE_HEADS,), jnp.float32) ** steps_of(key_of[6], (KEY_VALUE_HEADS,), ((0, 4),), -0.2, 0.2), -2.0, 1.5)
    key_cache = draw_key_cache(jax.random.fold_in(key_of[15], 71), 0)
    value_cache = centred(key_of[8], (BATCH_SEQUENCES, CACHE_LENGTH, KEY_VALUE_HEADS * HD), 1.0, 6.0, ((1, 8), (2, 4)))
    decay_to_end = draw_decay_to_end(jax.random.fold_in(key_of[15], 71), 0)
    w_output = centred(key_of[10], (QH * HD, D), (QH * HD) ** -0.5, 0.109375, ((0, 4), (1, 8)))
    mid_gain = jnp.clip(1.0 + 0.18 * jax.random.normal(key_of[11], (D,), jnp.float32), 0.1, 1.9)
    w_gate = centred(key_of[12], (D, FF), D ** -0.5, 0.09375, ((0, 8), (1, 4)))
    w_up = centred(key_of[13], (D, FF), D ** -0.5, 0.09375, ((0, 8), (1, 4)))
    w_down = centred(key_of[14], (FF, D), FF ** -0.5, 0.0546875, ((0, 4), (1, 8)))
    return {"hidden_in": hidden_in, "pre_gain": pre_gain, "w_query": w_query, "w_key": w_key, "w_value": w_value, "w_forget": w_forget, "forget_bias": forget_bias, "key_cache": key_cache, "value_cache": value_cache, "decay_to_end": decay_to_end, "w_output": w_output, "mid_gain": mid_gain, "w_gate": w_gate, "w_up": w_up, "w_down": w_down}


norm_eps = 1e-06

def grouped_sum(left, weight):
    groups = N_TP
    left_three = left.reshape(left.shape[0], groups, -1).astype(jnp.float32)
    weight_three = weight.reshape(groups, -1, weight.shape[1]).astype(jnp.float32)
    partial_terms = jnp.einsum('btk,tkd->btd', left_three, weight_three)
    rounded = lax.optimization_barrier(partial_terms.astype(jnp.bfloat16))
    return lax.optimization_barrier(jnp.sum(rounded.astype(jnp.float32), axis=1))

def attend_one(operands):
    query_b, keys_b, values_b, decay_b, key_own, value_own, log_b = operands
    score_scale = HD ** (-0.5)
    key_rows = keys_b.reshape(CACHE_LENGTH, KEY_VALUE_HEADS, HD).astype(jnp.float32)
    value_rows = values_b.reshape(CACHE_LENGTH, KEY_VALUE_HEADS, HD).astype(jnp.float32)
    query_f = query_b.astype(jnp.float32)
    scores = jnp.einsum('gqd,lgd->gql', query_f, key_rows) * score_scale
    scores = scores + log_b[:, None, None] + decay_b[:, None, :]
    own_score = jnp.einsum('gqd,gd->gq', query_f, key_own.astype(jnp.float32)) * score_scale
    largest = jnp.maximum(lax.optimization_barrier(jnp.max(scores, axis=2)), own_score)
    weights = jnp.exp(scores - largest[:, :, None])
    own_weight = jnp.exp(own_score - largest)
    total = lax.optimization_barrier(jnp.sum(weights, axis=2)) + own_weight
    rounded = lax.optimization_barrier(weights.astype(jnp.bfloat16))
    mixed = jnp.einsum('gql,lgd->gqd', rounded.astype(jnp.float32), value_rows)
    mixed = mixed + own_weight[:, :, None] * value_own.astype(jnp.float32)[:, None, :]
    return mixed / total[:, :, None]

def reference(hidden_in, pre_gain, w_query, w_key, w_value, w_forget, forget_bias, key_cache, value_cache, decay_to_end, w_output, mid_gain, w_gate, w_up, w_down):
    group_size = QH // KEY_VALUE_HEADS
    x_float = hidden_in.astype(jnp.float32)
    inv_rms = lax.rsqrt(lax.optimization_barrier(jnp.mean(x_float * x_float, axis=1, keepdims=True)) + norm_eps)
    scaled = (x_float * pre_gain).astype(jnp.bfloat16)
    query = (jnp.dot(scaled, w_query, preferred_element_type=jnp.float32) * inv_rms).astype(jnp.bfloat16)
    key_new = (jnp.dot(scaled, w_key, preferred_element_type=jnp.float32) * inv_rms).astype(jnp.bfloat16)
    value_new = (jnp.dot(scaled, w_value, preferred_element_type=jnp.float32) * inv_rms).astype(jnp.bfloat16)
    log_new = jax.nn.log_sigmoid(jnp.dot(scaled, w_forget, preferred_element_type=jnp.float32) * inv_rms + forget_bias)
    attended = lax.map(attend_one, (query.reshape(BATCH_SEQUENCES, KEY_VALUE_HEADS, group_size, HD), key_cache, value_cache, decay_to_end, key_new.reshape(BATCH_SEQUENCES, KEY_VALUE_HEADS, HD), value_new.reshape(BATCH_SEQUENCES, KEY_VALUE_HEADS, HD), log_new))
    attended = attended.reshape(BATCH_SEQUENCES, QH * HD).astype(jnp.bfloat16)
    projected = grouped_sum(attended, w_output)
    mid_float = x_float + projected
    mid_inv = lax.rsqrt(lax.optimization_barrier(jnp.mean(mid_float * mid_float, axis=1, keepdims=True)) + norm_eps)
    mid_scaled = (mid_float * mid_gain).astype(jnp.bfloat16)
    gate = jnp.dot(mid_scaled, w_gate, preferred_element_type=jnp.float32) * mid_inv
    upward = jnp.dot(mid_scaled, w_up, preferred_element_type=jnp.float32) * mid_inv
    hidden_units = (jax.nn.silu(gate) * upward).astype(jnp.bfloat16)
    lowered = grouped_sum(hidden_units, w_down)
    return mid_float + lowered
```

```python
import jax
import jax.numpy as jnp
from jax import lax
from jax.experimental import pallas as pl
from jax.experimental.pallas import tpu as pltpu
from jax.sharding import PartitionSpec as P

D = 4096
QH = 48
KEY_VALUE_HEADS = 16
HD = 64

norm_eps = 1e-06
AG_MODE = {"tp": "ag", "kv": "a2a"}
A2A_MODE = {"tp": "a2a", "kv": "a2a"}


def shifted(x, axis, shift):
    n = lax.axis_size(axis)
    return lax.ppermute(x, axis, [(i, (i + shift) % n) for i in range(n)])


def from_all(x, axis):
    n = lax.axis_size(axis)
    if AG_MODE[axis] == "perm":
        return [x] + [shifted(x, axis, s) for s in range(1, n)]
    if AG_MODE[axis] == "a2a":
        y = lax.all_to_all(jnp.broadcast_to(x[None], (n,) + x.shape), axis, 0, 0)
    else:
        y = lax.all_gather(x, axis)
    return [y[s] for s in range(n)]


def in_order(parts, axis, dim):
    n = lax.axis_size(axis)
    if AG_MODE[axis] != "perm":
        return jnp.concatenate(parts, axis=dim)
    size = parts[0].shape[dim]
    rising = parts[::-1]
    doubled = jnp.concatenate(rising + rising, axis=dim)
    me = lax.axis_index(axis)
    return lax.dynamic_slice_in_dim(doubled, (n - 1 - me) * size, n * size, dim)


def exchanged(x, axis, dim):
    n = lax.axis_size(axis)
    size = x.shape[dim] // n
    me = lax.axis_index(axis)
    if A2A_MODE[axis] == "perm":
        out = []
        for s in range(n):
            block = lax.dynamic_slice_in_dim(x, ((me + s) % n) * size, size, dim)
            out.append(shifted(block, axis, s) if s else block)
        return out
    y = lax.all_to_all(x, axis, dim, dim, tiled=True)
    return [lax.slice_in_dim(y, s * size, (s + 1) * size, axis=dim) for s in range(n)]


def total_of(parts):
    result = parts[0].astype(jnp.float32)
    for part in parts[1:]:
        result = result + part.astype(jnp.float32)
    return result


MANY = 8
SLOTS = 16


def terms_of(x):
    high = x.astype(jnp.bfloat16).astype(jnp.float32)
    rest = x - high
    middle = rest.astype(jnp.bfloat16).astype(jnp.float32)
    return high, middle, rest - middle


def attend_kernel(q_ref, k_ref, v_ref, d_ref, out_ref, q_f, rows_f):
    step = pl.program_id(0)
    many, kv_here, positions = d_ref.shape
    wide = k_ref.shape[2]
    group = q_ref.shape[1] // wide
    f32, bf16 = jnp.float32, jnp.bfloat16

    @pl.when(step == 0)
    def _():
        q_f[...] = q_ref[...].astype(f32)

    slot = lax.broadcasted_iota(jnp.int32, (SLOTS, wide), 0)
    head = lax.broadcasted_iota(jnp.int32, (SLOTS, wide), 1) // HD
    mine = [slot == q * kv_here + head for q in range(group)]
    of_slot = lax.broadcasted_iota(jnp.int32, (SLOTS, positions), 0) % kv_here
    lane = lax.broadcasted_iota(jnp.int32, (SLOTS, 128), 1)
    slot_s = lax.broadcasted_iota(jnp.int32, (SLOTS, 128), 0)
    queries = q_f[...]
    row_of = lax.broadcasted_iota(jnp.int32, queries.shape, 0)
    scores = []
    for n in range(many):
        q_row = jnp.sum(
            jnp.where(row_of == step * many + n, queries, 0.0), axis=0, keepdims=True
        )
        spread = jnp.zeros((SLOTS, wide), f32)
        for q in range(group):
            spread = jnp.where(mine[q], q_row[:, q * wide : (q + 1) * wide], spread)
        scores.append(
            lax.dot_general(
                (spread * HD ** (-0.5)).astype(bf16),
                k_ref[n],
                (((1,), (1,)), ((), ())),
                preferred_element_type=f32,
            )
        )
    tops, totals, weights = [], [], []
    for n in range(many):
        decay = jnp.broadcast_to(d_ref[n, 0:1, :], (SLOTS, positions))
        for g in range(1, kv_here):
            decay = jnp.where(of_slot == g, d_ref[n, g : g + 1, :], decay)
        shifted_scores = scores[n] + decay
        top = jnp.max(shifted_scores, axis=1, keepdims=True)
        weight = jnp.exp(shifted_scores - top)
        tops.append(top)
        totals.append(jnp.sum(weight, axis=1, keepdims=True))
        weights.append(weight.astype(bf16))
    accs = [jnp.dot(weights[n], v_ref[n], preferred_element_type=f32) for n in range(many)]
    result = rows_f[...]
    row_out = lax.broadcasted_iota(jnp.int32, result.shape, 0)
    for n in range(many):
        pieces = [jnp.sum(jnp.where(m, accs[n], 0.0), axis=0, keepdims=True) for m in mine]
        stats = jnp.zeros((SLOTS, 128), f32)
        for k, term in enumerate(terms_of(tops[n]) + terms_of(totals[n])):
            stats = jnp.where(lane == k * SLOTS + slot_s, term, stats)
        pieces.append(jnp.sum(stats, axis=0, keepdims=True))
        packed_row = jnp.concatenate(pieces, axis=1)
        result = jnp.where(row_out == step * many + n, packed_row, result)
    rows_f[...] = result

    @pl.when(step == pl.num_programs(0) - 1)
    def _():
        packed = rows_f[...].astype(bf16)
        for s in range(out_ref.shape[0]):
            out_ref[s] = packed


def attend(query, keys, values, decay, copies):
    rows, positions, wide = keys.shape
    cols = query.shape[1] + 128
    many = MANY
    return pl.pallas_call(
        attend_kernel,
        grid=(rows // many,),
        in_specs=[
            pl.BlockSpec(query.shape, lambda b: (0, 0)),
            pl.BlockSpec((many, positions, wide), lambda b: (b, 0, 0)),
            pl.BlockSpec((many, positions, wide), lambda b: (b, 0, 0)),
            pl.BlockSpec((many,) + decay.shape[1:], lambda b: (b, 0, 0)),
        ],
        out_specs=pl.BlockSpec((copies, rows, cols), lambda b: (0, 0, 0)),
        out_shape=jax.ShapeDtypeStruct((copies, rows, cols), jnp.bfloat16),
        scratch_shapes=[
            pltpu.VMEM(query.shape, jnp.float32),
            pltpu.VMEM((rows, cols), jnp.float32),
        ],
    )(query, keys, values, decay)


def project_kernel(x_ref, gain_ref, q_ref, k_ref, v_ref, f_ref, out_ref):
    f32 = jnp.float32
    x = x_ref[...].astype(f32)
    scaled = (x * gain_ref[...]).astype(jnp.bfloat16)
    parts = [
        jnp.dot(scaled, ref[...], preferred_element_type=f32) for ref in (q_ref, k_ref, v_ref)
    ]
    forget = jnp.dot(scaled, f_ref[...], preferred_element_type=f32)
    square = jnp.sum(x * x, axis=1, keepdims=True)
    gap = jnp.zeros((x.shape[0], 127 - forget.shape[1]), f32)
    parts.append(jnp.concatenate([forget, gap, square], axis=1))
    packed = jnp.concatenate(parts, axis=1)
    own_rows = out_ref.shape[1]
    for s in range(out_ref.shape[0]):
        out_ref[s] = packed[s * own_rows : (s + 1) * own_rows]


def joined(stats, first):
    return sum(stats[:, (first + k) * SLOTS : (first + k + 1) * SLOTS] for k in range(3))


def combine_kernel(got_ref, own_ref, w_ref, out_ref):
    sources, rows, cols = got_ref.shape
    q_cols = cols - 128
    f32 = jnp.float32
    wide = own_ref.shape[1] - q_cols - 128
    group = q_cols // wide
    kv_here = wide // HD
    own = joined(own_ref[:, q_cols + wide :].astype(f32), 0)
    stats = [got_ref[s, :, q_cols:].astype(f32) for s in range(sources)]
    maxima = [joined(stat, 0) for stat in stats]
    top = own
    for value in maxima:
        top = jnp.maximum(top, value)
    factors = [jnp.exp(value - top) for value in maxima]
    own_weight = jnp.exp(own - top)
    total = own_weight
    for factor, stat in zip(factors, stats):
        total = total + factor * joined(stat, 3)
    inverse = 1.0 / total
    ones = (
        lax.broadcasted_iota(jnp.int32, (SLOTS, q_cols), 1) // HD
        == lax.broadcasted_iota(jnp.int32, (SLOTS, q_cols), 0)
    ).astype(f32)
    shares = jnp.concatenate([f * inverse for f in factors + [own_weight]], axis=0)
    shares = jnp.dot(shares, ones, precision=lax.Precision.HIGHEST, preferred_element_type=f32)
    value_own = own_ref[:, q_cols : q_cols + wide].astype(f32)
    attended = shares[sources * rows :] * jnp.concatenate([value_own] * group, axis=1)
    for s in range(sources):
        attended = attended + shares[s * rows : (s + 1) * rows] * got_ref[s, :, :q_cols].astype(f32)
    in_heads = [
        attended[:, (q * kv_here + g) * HD : (q * kv_here + g + 1) * HD]
        for g in range(kv_here)
        for q in range(group)
    ]
    attended = jnp.concatenate(in_heads, axis=1).astype(jnp.bfloat16)
    out_ref[...] = jnp.dot(attended, w_ref[...], preferred_element_type=f32).astype(jnp.bfloat16)


def on_device(
    hidden_in,
    pre_gain,
    w_query,
    w_key,
    w_value,
    w_forget,
    forget_bias,
    key_cache,
    value_cache,
    decay_to_end,
    w_output,
    mid_gain,
    w_gate,
    w_up,
    w_down,
):
    rows = hidden_in.shape[0]
    kv_here = decay_to_end.shape[1]
    group = QH // KEY_VALUE_HEADS
    heads = kv_here * group
    q_cols = heads * HD
    k_cols = kv_here * HD
    n_kv = lax.axis_size("kv")
    own_rows = rows // n_kv
    tp_pos = lax.axis_index("tp")
    score_scale = HD ** (-0.5)
    f32, bf16 = jnp.float32, jnp.bfloat16

    col_block = in_order(from_all(hidden_in, "tp"), "tp", 1).astype(f32)
    first = pl.pallas_call(
        project_kernel,
        out_shape=jax.ShapeDtypeStruct((n_kv, own_rows, q_cols + 2 * k_cols + 128), f32),
    )(col_block.astype(bf16), pre_gain[None], w_query, w_key, w_value, w_forget)
    sums = total_of(exchanged(first, "kv", 0))[0]
    inv_rms = lax.rsqrt(sums[:, -1:] / D + norm_eps)
    q_own = (sums[:, :q_cols] * inv_rms).astype(bf16)
    k_own = (sums[:, q_cols : q_cols + k_cols] * inv_rms).astype(bf16)
    v_own = (sums[:, q_cols + k_cols : q_cols + 2 * k_cols] * inv_rms).astype(bf16)
    start = q_cols + 2 * k_cols
    forget = lax.dynamic_slice_in_dim(sums, start + tp_pos * kv_here, kv_here, 1)
    log_own = jax.nn.log_sigmoid(forget * inv_rms + forget_bias)
    q_four = q_own.reshape(own_rows, kv_here, group, HD)
    k_four = k_own.astype(f32).reshape(own_rows, kv_here, 1, HD)
    own_score = jnp.sum(q_four.astype(f32) * k_four, axis=3) * score_scale
    own_score = jnp.swapaxes(own_score - log_own[:, :, None], 1, 2).reshape(own_rows, heads)
    own_score = jnp.pad(own_score, ((0, 0), (0, SLOTS - heads)))
    q_slots = jnp.swapaxes(q_four, 1, 2).reshape(own_rows, q_cols)
    high = own_score.astype(bf16)
    rest = own_score - high.astype(f32)
    middle = rest.astype(bf16)
    low = (rest - middle.astype(f32)).astype(bf16)
    low = jnp.pad(low, ((0, 0), (0, 128 - 3 * SLOTS)))
    own = jnp.concatenate([q_slots, v_own, high, middle, low], axis=1)
    own_all = lax.all_to_all(jnp.broadcast_to(own[None], (n_kv,) + own.shape), "kv", 0, 0)
    own_all = own_all.reshape(rows, -1)
    packed = attend(own_all[:, :q_cols], key_cache, value_cache, decay_to_end, n_kv)
    got = lax.all_to_all(packed, "kv", 0, 0)
    out_part = pl.pallas_call(
        combine_kernel, out_shape=jax.ShapeDtypeStruct((rows, w_output.shape[1]), bf16)
    )(got, own_all, w_output)
    mid_block = col_block + total_of(from_all(out_part, "tp"))
    mine = hidden_in.shape[1]
    residual_mine = lax.dynamic_slice_in_dim(mid_block, tp_pos * mine, mine, 1)
    mid_scaled = (mid_block * mid_gain).astype(bf16)
    mid_square = jnp.sum(mid_block * mid_block, axis=1, keepdims=True)
    gate_part = jnp.dot(mid_scaled, w_gate, preferred_element_type=f32).astype(bf16)
    up_part = jnp.dot(mid_scaled, w_up, preferred_element_type=f32).astype(bf16)
    high = mid_square.astype(bf16)
    rest = mid_square - high.astype(f32)
    middle = rest.astype(bf16)
    low = (rest - middle.astype(f32)).astype(bf16)
    second = jnp.concatenate(
        [gate_part, up_part, jnp.pad(high, ((0, 0), (0, 125))), middle, low], axis=1
    )
    hid = gate_part.shape[1]
    sums = total_of(exchanged(second.reshape(n_kv, own_rows, -1), "kv", 0))[0]
    mid_total = sums[:, 2 * hid : 2 * hid + 1] + sums[:, -2:-1] + sums[:, -1:]
    mid_inv = lax.rsqrt(mid_total / D + norm_eps)
    gate = sums[:, :hid] * mid_inv
    up = sums[:, hid : 2 * hid] * mid_inv
    hidden_own = (jax.nn.silu(gate) * up).astype(bf16)
    hidden_units = in_order(from_all(hidden_own, "kv"), "kv", 0)
    down_part = jnp.dot(hidden_units, w_down, preferred_element_type=f32).astype(bf16)
    down_sum = total_of(from_all(down_part, "tp"))
    return residual_mine + lax.dynamic_slice_in_dim(down_sum, tp_pos * mine, mine, 1)


def solution(mesh):
    in_specs = (
        P(None, ("kv", "tp")),
        P("kv"),
        P("kv", "tp"),
        P("kv", "tp"),
        P("kv", "tp"),
        P("kv", None),
        P("tp"),
        P(None, "kv", "tp"),
        P(None, "kv", "tp"),
        P(None, "tp", "kv"),
        P("tp", "kv"),
        P("kv"),
        P("kv", "tp"),
        P("kv", "tp"),
        P("tp", "kv"),
    )
    out_specs = P(None, ("kv", "tp"))
    return jax.shard_map(
        on_device, mesh=mesh, in_specs=in_specs, out_specs=out_specs, check_vma=False
    )
```
